32 devices in a mesh: sp: 8 (over z, y), tp: 4 (over x, core).
Axes of the slice: x: 2, y: 2, z: 4, core: 2. Of those that a mesh axis runs over, the one named last changes fastest.
Arguments:
- conv_value: bfloat16 [4096, 2048], P('sp', 'tp'), may hold values from -6 to 6
- conv_gate: bfloat16 [4096, 2048], P('sp', 'tp'), may hold values from -6 to 6
- conv_taps: float32 [31, 2048], P(None, 'tp'), as said below
- channel_gain: float32 [2048], P('tp'), may hold values from 0.1 to 1.9
- point_weight: bfloat16 [2048, 2048], replicated, may hold values from -0.125 to 0.125
- residual_in: bfloat16 [4096, 2048], P(('sp', 'tp')), may hold values from -3 to 3
- first_gain: float32 [2048], replicated, may hold values from 0.1 to 1.9
- second_gain: float32 [2048], replicated, may hold values from 0.1 to 1.9
- routes: int32 [4096, 2], P(('sp', 'tp')), may hold values from 0 to 31, all different within a row; in each aligned block of 128 rows (0 to 127, 128 to 255, ...) at most 16 rows name the same one
- route_score: float32 [4096, 2], P(('sp', 'tp')), may hold values from 0.1 to 1
- expert_gate: bfloat16 [32, 2048, 1024], P(('sp', 'tp')), may hold values from -0.125 to 0.125
- expert_up: bfloat16 [32, 2048, 1024], P(('sp', 'tp')), may hold values from -0.125 to 0.125
- expert_down: bfloat16 [32, 1024, 2048], P(('sp', 'tp')), may hold values from -0.1875 to 0.1875
Outputs:
- layer_out: bfloat16 [4096, 2048], P(('sp', 'tp'))
The draws below stay inside these ranges and needn't reach their ends.
Inputs may be any that keep to these rules, and one draw needn't show every extreme that they name: `routes`: among the 128 rows of one device (aligned blocks of rows), no expert is named more than 16 times, a bound that some block reaches; a row names 2 different experts. conv_taps have independent entries, with scales that differ from channel to channel.
All inputs are finite; a program needn't handle non-finite values.
Results may differ from the reference program's by a relative error of at most 0.013.
Values may be sent and summed in bfloat16 or wider, within the bound.
A program may use at most 128 MiB of HBM per device.

```python
import math
import jax
import jax.numpy as jnp
import numpy as np
from jax import lax

D = 2048
FF = 1024
KW = 31
TOP = 2
TOKENS = 4096
ROWS = 128
EXPERTS = 32
MOST = 16


def draw_conv_taps(key, part):
    base_key = jax.random.fold_in(key, 11)
    tap_key, scale_key = jax.random.split(base_key)
    position = jnp.arange(D, dtype=jnp.float32) / D
    rising = 4.0 ** position
    taps = jax.random.normal(tap_key, (KW, D), jnp.float32)
    factor = jnp.exp(jax.random.uniform(scale_key, (1, D), jnp.float32, -0.7, 0.7))
    return (taps * factor * rising[None, :] * (0.5 / KW ** 0.5)).astype(jnp.float32)


def level_of(own_key, dims, shards, smallest, largest):
    factor_of = 1.0
    for dim, parts in shards:
        draws = jax.random.uniform(jax.random.fold_in(jax.random.fold_in(own_key, 6), dim), (parts,), jnp.float32, smallest / len(shards), largest / len(shards))
        factor_of = factor_of * jnp.repeat(jnp.exp(draws), dims[dim] // parts).reshape((-1,) + (1,) * (len(dims) - 1 - dim))
    return factor_of


def routed_block(own_key, own, number, rows, count, top, limit, slope):
    order = jax.random.permutation(own_key, count)
    packed, ordinary = load_shares(count, rows * top, limit, slope, True), load_shares(count, rows * top, limit, slope, False)
    places = jnp.arange(count)

    def named(lengths, offset_by):
        used = int((lengths > 0).sum())
        fixed = max(1, used // 4)
        shifted = fixed + (places - fixed + offset_by * (used - fixed)) % max(1, count - fixed)
        return jnp.zeros((count,), jnp.int32).at[order[jnp.where(places < fixed, places, shifted)]].set(jnp.asarray(lengths, jnp.int32))

    lengths = jnp.where(number % 4 == 0, named(packed, number // 4), named(ordinary, number - number // 4 - 1))
    mixed = jax.random.permutation(jax.random.fold_in(own, 3), count)
    source_of, taker = mixed[0:count // 2 * 2:2], mixed[1:count // 2 * 2:2]
    room = jnp.minimum(lengths[source_of] - 1, limit - lengths[taker]) // 2
    room = jnp.where((source_of == order[0]) | (taker == order[0]) | (lengths[taker] == 0), 0, jnp.maximum(room, 0))
    shifted = jax.random.randint(jax.random.fold_in(own, 4), (count // 2,), 0, 1 << 20) % (room + 1)
    lengths = lengths.at[source_of].add(-shifted).at[taker].add(shifted)
    labels = jnp.searchsorted(jnp.cumsum(lengths), jnp.arange(rows * top), side="right").astype(jnp.int32)
    table = labels.reshape(top, rows).T
    table = table[jax.random.permutation(jax.random.fold_in(own, 1), rows)]
    offset_by = jax.random.randint(jax.random.fold_in(own, 2), (rows, 1), 0, top)
    return jnp.take_along_axis(table, (jnp.arange(top)[None, :] + offset_by) % top, axis=1)


def load_shares(number_of, total, bound, skew, full):
    weights = [(1 << 20) // math.isqrt(standing ** skew) + 1 for standing in range(1, number_of + 1)]
    largest = bound if full else min(bound, max(-(-total // number_of), total * weights[0] // sum(weights)))
    least = 1 if total - largest >= number_of - 1 else 0
    given, rest = [largest] + [least] * (number_of - 1), total - largest - least * (number_of - 1)
    while rest > 0:
        free = [i for i in range(1, number_of) if given[i] < largest] or [i for i in range(1, number_of) if given[i] < bound]
        pool, budget = sum([weights[i] for i in free]), rest
        for i in free:
            more = min(bound - given[i], max(1, budget * weights[i] // pool), rest)
            given[i] = given[i] + more
            rest = rest - more
    return np.array(given)


def gaussian(own_key, shape, deviation, bound, pieces=(), kind=jnp.bfloat16):
    entries = jax.random.normal(own_key, shape, jnp.float32) * deviation
    if len(pieces) > 0:
        entries = level_of(own_key, shape, pieces, -0.22, 0.18) * entries
    return jnp.clip(entries, min=-bound, max=bound).astype(kind)


def setup_inputs(seed: int = 0) -> dict:
    splits = jax.random.split(jax.random.key(seed), 14)
    conv_value = gaussian(splits[0], (TOKENS, D), 1.0, 6.0, ((0, 8), (1, 4)))
    conv_gate = gaussian(splits[1], (TOKENS, D), 1.0, 6.0, ((0, 8), (1, 4)))
    conv_taps = draw_conv_taps(jax.random.fold_in(splits[13], 71), 0)
    channel_gain = jnp.clip(1.0 + 0.18 * jax.random.normal(splits[3], (D,), jnp.float32), 0.1, 1.9)
    point_weight = gaussian(splits[4], (D, D), D ** -0.5, 0.125)
    residual_in = gaussian(splits[5], (TOKENS, D), 0.5, 3.0, ((0, 32),))
    first_gain = jnp.clip(1.0 + 0.18 * jax.random.normal(splits[6], (D,), jnp.float32), 0.1, 1.9)
    second_gain = jnp.clip(1.0 + 0.18 * jax.random.normal(splits[7], (D,), jnp.float32), 0.1, 1.9)
    routes_keys = jax.random.split(jax.random.fold_in(splits[8], 1), TOKENS // ROWS)
    routes_turns = jax.random.permutation(jax.random.fold_in(splits[8], 3), TOKENS // ROWS)
    routes = jax.vmap(lambda own, number: routed_block(jax.random.fold_in(splits[8], 2), own, number, ROWS, EXPERTS, TOP, MOST, 0))(routes_keys, routes_turns).reshape((TOKENS, TOP))
    route_score = jnp.clip(0.1 + 0.9 * jax.random.uniform(splits[9], (TOKENS, TOP), jnp.float32) ** level_of(splits[9], (TOKENS, TOP), ((0, 32),), -0.2, 0.2), 0.1, 1.0)
    expert_gate = gaussian(splits[10], (EXPERTS, D, FF), D ** -0.5, 0.125, ((0, 32),))
    expert_up = gaussian(splits[11], (EXPERTS, D, FF), D ** -0.5, 0.125, ((0, 32),))
    expert_down = gaussian(splits[12], (EXPERTS, FF, D), FF ** -0.5, 0.1875, ((0, 32),))
    return dict(conv_value=conv_value, conv_gate=conv_gate, conv_taps=conv_taps, channel_gain=channel_gain, point_weight=point_weight, residual_in=residual_in, first_gain=first_gain, second_gain=second_gain, routes=routes, route_score=route_score, expert_gate=expert_gate, expert_up=expert_up, expert_down=expert_down)


block_rows = 32
residual_scale = 8.0 ** 0.25

def token_norm(values, gain):
    middle = lax.optimization_barrier(jnp.mean(values, axis=-1, keepdims=True))
    centred = values - middle
    spread = lax.optimization_barrier(jnp.mean(centred * centred, axis=-1, keepdims=True))
    return centred * lax.rsqrt(spread + 1e-05) * gain

def reference(conv_value, conv_gate, conv_taps, channel_gain, point_weight, residual_in, first_gain, second_gain, routes, route_score, expert_gate, expert_up, expert_down):
    glu = conv_value.astype(jnp.float32) * jax.nn.sigmoid(conv_gate.astype(jnp.float32))
    padded_glu = jnp.concatenate([jnp.zeros((KW - 1, D), glu.dtype), glu], axis=0)
    conv = jnp.zeros((TOKENS, D), glu.dtype)
    for tap in range(KW):
        conv = conv + conv_taps[tap][None, :].astype(glu.dtype) * padded_glu[tap:tap + TOKENS]
    middle = lax.optimization_barrier(jnp.mean(conv, axis=1, keepdims=True))
    spread = lax.optimization_barrier(jnp.mean(conv * conv, axis=1, keepdims=True)) - middle * middle
    normed = (conv - middle) * lax.rsqrt(spread + 1e-05) * channel_gain
    act = (normed * jax.nn.sigmoid(normed)).astype(jnp.bfloat16)
    mix = jnp.dot(act, point_weight, preferred_element_type=jnp.float32)
    first = token_norm(residual_scale * residual_in.astype(jnp.float32) + mix, first_gain).astype(jnp.bfloat16)
    total = TOKENS * TOP
    flat_e = routes.reshape(-1).astype(jnp.int32)
    flat_t = (jnp.arange(total, dtype=jnp.int32) // TOP).astype(jnp.int32)
    order = jnp.argsort(flat_e, stable=True).astype(jnp.int32)
    sorted_e = flat_e[order]
    sorted_t = flat_t[order]
    counts = lax.optimization_barrier(jnp.sum((flat_e[:, None] == jnp.arange(EXPERTS, dtype=jnp.int32)[None, :]).astype(jnp.int32), axis=0))
    padded = (counts + block_rows - 1) // block_rows * block_rows
    begin = jnp.cumsum(counts) - counts
    pad_end = jnp.cumsum(padded)
    pad_begin = pad_end - padded
    dest = (pad_begin[sorted_e] + jnp.arange(total, dtype=jnp.int32) - begin[sorted_e]).astype(jnp.int32)
    n_rows = (total + block_rows - 1) // block_rows * block_rows + EXPERTS * block_rows
    n_blocks = n_rows // block_rows
    row_tok = jnp.full((n_rows,), TOKENS, jnp.int32).at[dest].set(sorted_t)
    block_expert = jnp.minimum(jnp.searchsorted(pad_end, jnp.arange(n_blocks, dtype=jnp.int32) * block_rows, side='right'), EXPERTS - 1).astype(jnp.int32)
    padded_first = jnp.concatenate([first, jnp.zeros((1, D), jnp.bfloat16)], axis=0)

    def run_block(inputs):
        tokens_idx, expert = inputs
        rows_in = padded_first[tokens_idx]
        gate = jnp.dot(rows_in, expert_gate[expert], preferred_element_type=jnp.float32)
        upper = jnp.dot(rows_in, expert_up[expert], preferred_element_type=jnp.float32)
        hidden = (jax.nn.silu(gate) * upper).astype(jnp.bfloat16)
        return jnp.dot(hidden, expert_down[expert], preferred_element_type=jnp.float32).astype(jnp.bfloat16)
    answers = lax.map(run_block, (row_tok.reshape(n_blocks, block_rows), block_expert)).reshape(n_rows, D)
    per_assign = jnp.zeros((total, D), jnp.bfloat16).at[order].set(answers[dest])
    share = route_score / lax.optimization_barrier(jnp.sum(route_score, axis=1, keepdims=True))
    moe = lax.optimization_barrier(jnp.sum(share[:, :, None] * per_assign.reshape(TOKENS, TOP, D).astype(jnp.float32), axis=1))
    return token_norm(residual_scale * first.astype(jnp.float32) + moe, second_gain).astype(jnp.bfloat16)
```

```python
import functools

import jax
import jax.numpy as jnp
from jax import lax
from jax.experimental import pallas as pl
from jax.experimental.pallas import tpu as pltpu
from jax.sharding import PartitionSpec as P

residual_scale = 8.0**0.25
MESH = pl.DeviceIdType.MESH
VMEM = pl.BlockSpec(memory_space=pltpu.VMEM)


class Grid:
    def __init__(self, sp, tp):
        self.sp, self.tp = sp, tp
        self.planes = 4 if sp % 4 == 0 else 1
        self.inner = sp // self.planes
        self.peers = self.inner * tp

    def here(self):
        s, t = lax.axis_index("sp"), lax.axis_index("tp")
        return s // self.inner, (s % self.inner) * self.tp + t

    def device(self, plane, peer):
        return (plane * self.inner + peer // self.tp, peer % self.tp)

    def greet(self, plane, peer):
        barrier = pltpu.get_barrier_semaphore()
        for d in range(1, self.planes):
            other = self.device((plane + d) % self.planes, peer)
            pl.semaphore_signal(barrier, inc=1, device_id=other, device_id_type=MESH)
        for d in range(1, self.peers):
            other = self.device(plane, (peer + d) % self.peers)
            pl.semaphore_signal(barrier, inc=1, device_id=other, device_id_type=MESH)
        pl.semaphore_wait(barrier, self.planes - 1 + self.peers - 1)


def remote(src, dst, send, recv, device):
    return pltpu.make_async_remote_copy(
        src_ref=src, dst_ref=dst, send_sem=send, recv_sem=recv, device_id=device, device_id_type=MESH
    )


def experts_kernel(
    g, cap, parts, first, table, gain, w_gate, w_up, w_down, final, v_gate, v_up, v_down, hidden, out, tables, held,
    stage, back, sums, came, h2, share, blk_send, blk_recv, tab_send, tab_recv, row_send, row_recv, own_sem, ans_send,
    ans_recv, ans_own, sum_send, sum_recv, w_sem,
):
    plane, peer = g.here()
    last = g.planes - 1
    rows, width = first.shape
    slots = g.peers * cap
    part = width // parts
    above = g.device((plane + 1) % g.planes, peer)
    below = g.device((plane + last) % g.planes, peer)
    loads = [
        pltpu.make_async_copy(src.at[0], dst, w_sem.at[n])
        for n, (src, dst) in enumerate(((w_gate, v_gate), (w_up, v_up), (w_down, v_down)))
    ]
    for load in loads:
        load.start()
    held[plane] = first[...]
    tables[plane] = table[...]
    g.greet(plane, peer)

    def cols(c):
        return pl.ds(c * part, part)

    def mine(at):
        return pl.ds(pl.multiple_of(at * cap, cap), cap)

    def table_copy(b, way, own):
        src = table if own else tables.at[b]
        return remote(src, tables.at[b], tab_send.at[way, b], tab_recv.at[b], above if way == 0 else below)

    def block_copy(b, way, c, own):
        src = first.at[:, cols(c)] if own else held.at[b, :, cols(c)]
        return remote(
            src, held.at[b, :, cols(c)], blk_send.at[way, b, c], blk_recv.at[b, c], above if way == 0 else below
        )

    def has_way(way):
        return plane < last if way == 0 else plane > 0

    def near(s):
        return [(way, b, (b >= 0) & (b <= last)) for way, b in ((0, plane - s), (1, plane + s))]

    def numbers():
        number = lax.broadcasted_iota(jnp.int32, (slots, rows), 0) + plane * slots
        return number.astype(jnp.float32)

    def weigh(b):
        number = numbers()
        t = tables[b]
        weight = jnp.where(number == t[0:1], t[2:3], 0.0) + jnp.where(number == t[1:2], t[3:4], 0.0)
        weight = weight.T
        high = weight.astype(jnp.bfloat16)
        share[b, 0] = high
        share[b, 1] = (weight - high.astype(jnp.float32)).astype(jnp.bfloat16)

    def place(b, c):
        number = numbers()
        t = tables[b]
        pick = jnp.where((number == t[0:1]) | (number == t[1:2]), 1.0, 0.0).astype(jnp.bfloat16)
        picked = jnp.dot(pick, held[b, :, cols(c)], preferred_element_type=jnp.float32)
        stage[b, :, cols(c)] = picked.astype(jnp.bfloat16)
        for d in range(1, g.peers):
            row_copy(b, d, c).start()
        own_copy(b, c).start()

    def row_copy(b, d, c):
        to = (peer + d) % g.peers
        return remote(
            stage.at[b, mine(to), cols(c)],
            out.at[b, mine(peer), cols(c)],
            row_send.at[b, d, c],
            row_recv.at[b, d, c],
            g.device(plane, to),
        )

    def own_copy(b, c):
        return pltpu.make_async_copy(stage.at[b, mine(peer), cols(c)], out.at[b, mine(peer), cols(c)], own_sem.at[b, c])

    def ans_copy(b, d, c):
        to = (peer + d) % g.peers
        return remote(
            out.at[b, mine(to), cols(c)],
            back.at[b, mine(peer), cols(c)],
            ans_send.at[b, d, c],
            ans_recv.at[b, d, c],
            g.device(plane, to),
        )

    def ans_own_copy(b, c):
        return pltpu.make_async_copy(out.at[b, mine(peer), cols(c)], back.at[b, mine(peer), cols(c)], ans_own.at[b, c])

    def partial(b, c):
        ans_own_copy(b, c).wait()
        for d in range(1, g.peers):
            ans_copy(b, d, c).wait_recv()
        got = back[b, :, cols(c)]
        return jnp.dot(share[b, 0], got, preferred_element_type=jnp.float32) + jnp.dot(
            share[b, 1], got, preferred_element_type=jnp.float32
        )

    def sum_copy(b, way, c):
        return remote(
            sums.at[b, :, cols(c)],
            came.at[way, b, :, cols(c)],
            sum_send.at[b, c],
            sum_recv.at[way, b, c],
            above if way == 0 else below,
        )

    def chains(k):
        yield 0, k, k > plane, plane > 0
        yield 1, last - k, last - k < plane, plane < last

    cut = 256

    def expert(b):
        for c in range(parts):
            own_copy(b, c).wait()
            for d in range(1, g.peers):
                row_copy(b, d, c).wait_recv()

        def inner(n, carry):
            at = pl.ds(pl.multiple_of(n * cut, cut), cut)
            x = out[b]
            gate = jnp.dot(x, v_gate[:, at], preferred_element_type=jnp.float32)
            upper = jnp.dot(x, v_up[:, at], preferred_element_type=jnp.float32)
            hidden[:, at] = (gate * jax.nn.sigmoid(gate) * upper).astype(jnp.bfloat16)
            return carry

        lax.fori_loop(0, v_gate.shape[1] // cut, inner, 0)
        for c in range(parts):
            answer = jnp.dot(hidden[...], v_down[:, cols(c)], preferred_element_type=jnp.float32)
            out[b, :, cols(c)] = answer.astype(jnp.bfloat16)
            for d in range(1, g.peers):
                ans_copy(b, d, c).start()
            ans_own_copy(b, c).start()

    def experts_near(s):
        for way, b, valid in near(s):
            pl.when(valid)(functools.partial(expert, b))

    def combine(k, c):
        for way, b, valid, relayed in chains(k):

            @pl.when(valid & relayed)
            def _():
                total = partial(b, c)
                sum_copy(b, way, c).wait_recv()
                sums[b, :, cols(c)] = (total + came[way, b, :, cols(c)].astype(jnp.float32)).astype(jnp.bfloat16)
                sum_copy(b, way, c).start()

            @pl.when(valid & jnp.logical_not(relayed))
            def _():
                sums[b, :, cols(c)] = partial(b, c).astype(jnp.bfloat16)
                sum_copy(b, way, c).start()

    def arrive(s, c):
        for way, b, valid in near(s):

            @pl.when(valid)
            def _():
                if c == 0:
                    table_copy(b, way, False).wait_recv()

                    @pl.when(has_way(way))
                    def _():
                        table_copy(b, way, False).start()

                block_copy(b, way, c, False).wait_recv()

                @pl.when(has_way(way))
                def _():
                    block_copy(b, way, c, False).start()

                place(b, c)
                if c == 0:
                    weigh(b)

    for way in range(2):

        @pl.when(has_way(way))
        def _():
            table_copy(plane, way, True).start()
            for c in range(parts):
                block_copy(plane, way, c, True).start()

    for c in range(parts):
        place(plane, c)
    weigh(plane)
    for s in range(1, g.planes + 1):
        for c in range(parts):
            if s < g.planes:
                arrive(s, c)
            if s == 1 and c == parts - 2:
                for load in loads:
                    load.wait()
                expert(plane)
            if s > 1 and c == 0:
                experts_near(s - 1)
            if s == 2 and c == parts - 2:
                for n in range(parts):
                    h2[:, cols(n)] = residual_scale * first[:, cols(n)].astype(jnp.float32) + partial(plane, n)
            if s == g.planes:
                combine(s - 1, c)
            elif s > 1 and c == parts - 2:
                for n in range(parts // 2):
                    combine(s - 1, n)
            elif s > 1 and c == parts - 1:
                for n in range(parts // 2, parts):
                    combine(s - 1, n)

    for c in range(parts):
        for way in range(2):

            @pl.when(plane > 0 if way == 0 else plane < last)
            def _():
                sum_copy(plane, way, c).wait_recv()
                h2[:, cols(c)] += came[way, plane, :, cols(c)].astype(jnp.float32)

    final[...] = token_norm(h2[...], gain[...]).astype(jnp.bfloat16)
    for c in range(parts):
        for k in range(1, g.planes):
            for way, b, valid, relayed in chains(k):
                pl.when(valid)(lambda: sum_copy(b, way, c).wait_send())
        for b in range(g.planes):
            for d in range(1, g.peers):
                ans_copy(b, d, c).wait_send()
                row_copy(b, d, c).wait_send()
        for s in range(1, g.planes):
            for way, b, valid in near(s):
                pl.when(valid & has_way(way))(lambda: block_copy(b, way, c, False).wait_send())
        for way in range(2):
            pl.when(has_way(way))(lambda: block_copy(plane, way, c, True).wait_send())
    for s in range(1, g.planes):
        for way, b, valid in near(s):
            pl.when(valid & has_way(way))(lambda: table_copy(b, way, False).wait_send())
    for way in range(2):
        pl.when(has_way(way))(lambda: table_copy(plane, way, True).wait_send())


def experts(g, cap, first, table, gain, w_gate, w_up, w_down):
    rows, width = first.shape
    hidden = w_gate.shape[2]
    slots = g.peers * cap
    parts = 4
    dma = pltpu.SemaphoreType.DMA
    f32, bf16 = jnp.float32, jnp.bfloat16
    blocks, pairs = dma((g.planes, parts)), dma((g.planes, g.peers, parts))
    any_place = pl.BlockSpec(memory_space=pl.ANY)
    return pl.pallas_call(
        functools.partial(experts_kernel, g, cap, parts),
        name="experts",
        out_shape=jax.ShapeDtypeStruct((rows, width), bf16),
        in_specs=[VMEM] * 3 + [any_place] * 3,
        out_specs=VMEM,
        scratch_shapes=[
            pltpu.VMEM((width, hidden), bf16),
            pltpu.VMEM((width, hidden), bf16),
            pltpu.VMEM((hidden, width), bf16),
            pltpu.VMEM((slots, hidden), bf16),
            pltpu.VMEM((g.planes, slots, width), bf16),
            pltpu.VMEM((g.planes,) + table.shape, f32),
            pltpu.VMEM((g.planes, rows, width), bf16),
            pltpu.VMEM((g.planes, slots, width), bf16),
            pltpu.VMEM((g.planes, slots, width), bf16),
            pltpu.VMEM((g.planes, rows, width), bf16),
            pltpu.VMEM((2, g.planes, rows, width), bf16),
            pltpu.VMEM((rows, width), f32),
            pltpu.VMEM((g.planes, 2, rows, slots), bf16),
            dma((2, g.planes, parts)),
            blocks,
            dma((2, g.planes)),
            dma((g.planes,)),
            pairs,
            pairs,
            blocks,
            pairs,
            pairs,
            blocks,
            blocks,
            dma((2, g.planes, parts)),
            dma((3,)),
        ],
        compiler_params=pltpu.CompilerParams(collective_id=0, has_side_effects=True),
    )(first, table, gain, w_gate, w_up, w_down)


def front_kernel(
    sp, tp, value, gate, taps, gain, out, rim_v, rim_g, glu, conv, part1, part2, stat, stats, cols, stage,
    rim_send, rim_recv, stat_send, stat_recv, act_send, act_recv, own_sem,
):
    s, t = lax.axis_index("sp"), lax.axis_index("tp")
    tokens, width = value.shape
    kw = taps.shape[0]
    pad = rim_v.shape[0]
    rows = tokens // tp
    lead = pad - (kw - 1)
    tile = 64
    lane = 128

    barrier = pltpu.get_barrier_semaphore()
    for other in ((s + 1) % sp, (s + sp - 1) % sp):
        pl.semaphore_signal(barrier, inc=1, device_id=(other, t), device_id_type=MESH)
    for d in range(1, tp):
        pl.semaphore_signal(barrier, inc=1, device_id=(s, (t + d) % tp), device_id_type=MESH)
    pl.semaphore_wait(barrier, 2 + tp - 1)

    def rims():
        to = ((s + 1) % sp, t)
        tail = pl.ds(tokens - pad, pad)
        return (
            remote(value.at[tail], rim_v, rim_send.at[0], rim_recv.at[0], to),
            remote(gate.at[tail], rim_g, rim_send.at[1], rim_recv.at[1], to),
        )

    @pl.when(s < sp - 1)
    def _():
        for copy in rims():
            copy.start()

    def gated(v, g):
        return v.astype(jnp.float32) * jax.nn.sigmoid(g.astype(jnp.float32))

    def glu_tile(i, carry):
        at = pl.multiple_of(i * tile, tile)
        glu[pl.ds(pad + at, tile)] = gated(value[pl.ds(at, tile)], gate[pl.ds(at, tile)])
        return carry

    lax.fori_loop(0, tokens // tile, glu_tile, 0)

    def conv_tile(i, carry):
        at = pl.multiple_of(i * tile, tile)
        one = two = None
        for c in range(width // lane):
            lanes = pl.ds(c * lane, lane)
            total = None
            for r in range(8):
                piece = None
                extra = 8 if r else 0
                for m in range(pad // 8 + 1):
                    j = 8 * m + r - lead
                    if 0 <= j < kw:
                        term = taps[j : j + 1, lanes] * glu[pl.ds(at + 8 * m, tile + extra), lanes]
                        piece = term if piece is None else piece + term
                if piece is not None:
                    piece = piece[r : r + tile]
                    total = piece if total is None else total + piece
            conv[pl.ds(at, tile), lanes] = total
            one = total if one is None else one + total
            two = total * total if two is None else two + total * total
        part1[pl.ds(at, tile)] = one
        part2[pl.ds(at, tile)] = two
        return carry

    lax.fori_loop(1, tokens // tile, conv_tile, 0)

    @pl.when(s > 0)
    def _():
        for copy in rims():
            copy.wait_recv()
        glu[pl.ds(0, pad)] = gated(rim_v[...], rim_g[...])

    @pl.when(s == 0)
    def _():
        glu[pl.ds(0, pad)] = jnp.zeros((pad, width), jnp.float32)

    conv_tile(0, 0)

    ones = jnp.ones((8, lane), jnp.float32)

    def row_sums(part):
        return lax.dot_general(
            ones,
            part[...],
            (((1,), (1,)), ((), ())),
            precision=lax.Precision.HIGHEST,
            preferred_element_type=jnp.float32,
        )

    first_row = lax.broadcasted_iota(jnp.int32, (8, tokens), 0) == 0
    mine = jnp.where(first_row, row_sums(part1), row_sums(part2))
    stat[...] = mine

    def stat_copy(d):
        return remote(stat, stats.at[d], stat_send.at[d], stat_recv.at[d], (s, (t + d) % tp))

    for d in range(1, tp):
        stat_copy(d).start()
    for d in range(1, tp):
        stat_copy(d).wait_recv()
        mine = mine + stats[d]
    scaled = mine / (width * tp)
    middle = scaled[0:1]
    factor = lax.rsqrt(scaled[1:2] - middle * middle + 1e-05)
    cols[...] = jnp.where(first_row, middle, factor).T

    def act_copy(d):
        to = (t + d) % tp
        return remote(
            stage.at[d],
            out.at[:, pl.ds(pl.multiple_of(t * width, width), width)],
            act_send.at[d],
            act_recv.at[d],
            (s, to),
        )

    own = pltpu.make_async_copy(stage.at[0], out.at[:, pl.ds(pl.multiple_of(t * width, width), width)], own_sem)
    for d in list(range(1, tp)) + [0]:
        at = pl.multiple_of((t + d) % tp * rows, rows)
        side = cols[pl.ds(at, rows)]
        normed = (conv[pl.ds(at, rows)] - side[:, 0:1]) * side[:, 1:2] * gain[...]
        stage[d] = (normed * jax.nn.sigmoid(normed)).astype(jnp.bfloat16)
        if d:
            act_copy(d).start()
        else:
            own.start()
    own.wait()
    for d in range(1, tp):
        act_copy(d).wait()
        stat_copy(d).wait_send()

    @pl.when(s < sp - 1)
    def _():
        for copy in rims():
            copy.wait_send()


def front(sp, tp, value, gate, taps, gain):
    tokens, width = value.shape
    pad = -(-(taps.shape[0] - 1) // 16) * 16
    rows = tokens // tp
    dma = pltpu.SemaphoreType.DMA
    f32, bf16 = jnp.float32, jnp.bfloat16
    return pl.pallas_call(
        functools.partial(front_kernel, sp, tp),
        name="front",
        out_shape=jax.ShapeDtypeStruct((rows, width * tp), bf16),
        in_specs=[VMEM] * 4,
        out_specs=VMEM,
        scratch_shapes=[
            pltpu.VMEM((pad, width), bf16),
            pltpu.VMEM((pad, width), bf16),
            pltpu.VMEM((pad + tokens, width), f32),
            pltpu.VMEM((tokens, width), f32),
            pltpu.VMEM((tokens, 128), f32),
            pltpu.VMEM((tokens, 128), f32),
            pltpu.VMEM((8, tokens), f32),
            pltpu.VMEM((tp, 8, tokens), f32),
            pltpu.VMEM((tokens, 8), f32),
            pltpu.VMEM((tp, rows, width), bf16),
            dma((2,)),
            dma((2,)),
            dma((tp,)),
            dma((tp,)),
            dma((tp,)),
            dma((tp,)),
            dma,
        ],
        compiler_params=pltpu.CompilerParams(collective_id=2, has_side_effects=True),
    )(value, gate, taps, gain)


def token_norm(values, gain):
    middle = jnp.mean(values, axis=-1, keepdims=True)
    centred = values - middle
    spread = jnp.mean(centred * centred, axis=-1, keepdims=True)
    return centred * lax.rsqrt(spread + 1e-05) * gain


def per_device(
    conv_value,
    conv_gate,
    conv_taps,
    channel_gain,
    point_weight,
    residual_in,
    first_gain,
    second_gain,
    routes,
    route_score,
    expert_gate,
    expert_up,
    expert_down,
):
    owned = front(
        lax.axis_size("sp"), lax.axis_size("tp"), conv_value, conv_gate, conv_taps, channel_gain[None]
    )
    rows = owned.shape[0]
    mix = jnp.dot(owned, point_weight, preferred_element_type=jnp.float32)
    first = token_norm(residual_scale * residual_in.astype(jnp.float32) + mix, first_gain).astype(
        jnp.bfloat16
    )
    top = routes.shape[1]
    g = Grid(lax.axis_size("sp"), lax.axis_size("tp"))
    count = g.planes * g.peers
    most = max(2, 2 * rows * top // count)
    cap = -(-most // 16) * 16
    flat_e = routes.reshape(-1)
    onehot = (flat_e[:, None] == jnp.arange(count, dtype=jnp.int32)[None, :]).astype(jnp.int32)
    before = jnp.sum((jnp.cumsum(onehot, axis=0) - onehot) * onehot, axis=1)
    slot = (flat_e * cap + before).reshape(rows, top).astype(jnp.float32)
    share = route_score / jnp.sum(route_score, axis=1, keepdims=True)
    table = jnp.concatenate([slot, share, jnp.zeros((rows, 4), jnp.float32)], axis=1).T
    return experts(g, cap, first, table, second_gain[None], expert_gate, expert_up, expert_down)


def solution(mesh):
    in_specs = (
        P("sp", "tp"),
        P("sp", "tp"),
        P(None, "tp"),
        P("tp"),
        P(),
        P(("sp", "tp"), None),
        P(),
        P(),
        P(("sp", "tp"), None),
        P(("sp", "tp"), None),
        P(("sp", "tp"), None, None),
        P(("sp", "tp"), None, None),
        P(("sp", "tp"), None, None),
    )
    out_specs = P(("sp", "tp"), None)
    return jax.shard_map(
        per_device, mesh=mesh, in_specs=in_specs, out_specs=out_specs, check_vma=False
    )
```

```python
import functools

import jax
import jax.numpy as jnp
from jax import lax
from jax.experimental import pallas as pl
from jax.experimental.pallas import tpu as pltpu
from jax.sharding import PartitionSpec as P

residual_scale = 8.0**0.25
MESH = pl.DeviceIdType.MESH
VMEM = pl.BlockSpec(memory_space=pltpu.VMEM)


class Grid:
    def __init__(self, sp, tp):
        self.sp, self.tp = sp, tp
        self.planes = 4 if sp % 4 == 0 else 1
        self.inner = sp // self.planes
        self.peers = self.inner * tp

    def here(self):
        s, t = lax.axis_index("sp"), lax.axis_index("tp")
        return s // self.inner, (s % self.inner) * self.tp + t

    def device(self, plane, peer):
        return (plane * self.inner + peer // self.tp, peer % self.tp)

    def greet(self, plane, peer):
        barrier = pltpu.get_barrier_semaphore()
        for d in range(1, self.planes):
            other = self.device((plane + d) % self.planes, peer)
            pl.semaphore_signal(barrier, inc=1, device_id=other, device_id_type=MESH)
        for d in range(1, self.peers):
            other = self.device(plane, (peer + d) % self.peers)
            pl.semaphore_signal(barrier, inc=1, device_id=other, device_id_type=MESH)
        pl.semaphore_wait(barrier, self.planes - 1 + self.peers - 1)


def remote(src, dst, send, recv, device):
    return pltpu.make_async_remote_copy(
        src_ref=src, dst_ref=dst, send_sem=send, recv_sem=recv, device_id=device, device_id_type=MESH
    )


def experts_kernel(
    g, cap, parts, first, table, gain, w_gate, w_up, w_down, final, v_gate, v_up, v_down, hidden, out, tables, held,
    stage, back, sums, came, h2, share, blk_send, blk_recv, tab_send, tab_recv, row_send, row_recv, own_sem, ans_send,
    ans_recv, ans_own, sum_send, sum_recv, w_sem,
):
    plane, peer = g.here()
    last = g.planes - 1
    rows, width = first.shape
    slots = g.peers * cap
    part = width // parts
    at_end = (plane == 0) | (plane == last)
    loads = [
        pltpu.make_async_copy(src.at[0], dst, w_sem.at[n])
        for n, (src, dst) in enumerate(((w_gate, v_gate), (w_up, v_up), (w_down, v_down)))
    ]
    for load in loads:
        load.start()
    held[plane] = first[...]
    tables[plane] = table[...]
    g.greet(plane, peer)

    def cols(c):
        return pl.ds(c * part if isinstance(c, int) else pl.multiple_of(c * part, part), part)

    def toward(way):
        return g.device((plane + (last if way else 1)) % g.planes, peer)

    def mine(at):
        return pl.ds(pl.multiple_of(at * cap, cap), cap)

    def table_copy(b, way, own):
        src = table if own else tables.at[b]
        return remote(src, tables.at[b], tab_send.at[way, b], tab_recv.at[b], toward(way))

    def block_copy(b, way, c, own):
        src = first.at[:, cols(c)] if own else held.at[b, :, cols(c)]
        return remote(
            src, held.at[b, :, cols(c)], blk_send.at[way, b, c], blk_recv.at[b, c], toward(way)
        )

    def has_way(way):
        return plane < last if way == 0 else plane > 0

    def near(s):
        return [(way, b, (b >= 0) & (b <= last)) for way, b in ((0, plane - s), (1, plane + s))]

    def numbers():
        number = lax.broadcasted_iota(jnp.int32, (slots, rows), 0) + plane * slots
        return number.astype(jnp.float32)

    def weigh(b):
        number = numbers()
        t = tables[b]
        weight = jnp.where(number == t[0:1], t[2:3], 0.0) + jnp.where(number == t[1:2], t[3:4], 0.0)
        weight = weight.T
        high = weight.astype(jnp.bfloat16)
        share[b, 0] = high
        share[b, 1] = (weight - high.astype(jnp.float32)).astype(jnp.bfloat16)

    def place(b, c):
        number = numbers()
        t = tables[b]
        pick = jnp.where((number == t[0:1]) | (number == t[1:2]), 1.0, 0.0).astype(jnp.bfloat16)
        picked = jnp.dot(pick, held[b, :, cols(c)], preferred_element_type=jnp.float32)
        stage[b, :, cols(c)] = picked.astype(jnp.bfloat16)
        for d in range(1, g.peers):
            row_copy(b, d, c).start()
        own_copy(b, c).start()

    def row_copy(b, d, c):
        to = (peer + d) % g.peers
        return remote(
            stage.at[b, mine(to), cols(c)],
            out.at[b, mine(peer), cols(c)],
            row_send.at[b, d, c],
            row_recv.at[b, d, c],
            g.device(plane, to),
        )

    def own_copy(b, c):
        return pltpu.make_async_copy(stage.at[b, mine(peer), cols(c)], out.at[b, mine(peer), cols(c)], own_sem.at[b, c])

    def ans_copy(b, d, c):
        to = (peer + d) % g.peers
        return remote(
            out.at[b, mine(to), cols(c)],
            back.at[b, mine(peer), cols(c)],
            ans_send.at[b, d, c],
            ans_recv.at[b, d, c],
            g.device(plane, to),
        )

    def ans_own_copy(b, c):
        return pltpu.make_async_copy(out.at[b, mine(peer), cols(c)], back.at[b, mine(peer), cols(c)], ans_own.at[b, c])

    def partial(b, c):
        ans_own_copy(b, c).wait()
        for d in range(1, g.peers):
            ans_copy(b, d, c).wait_recv()
        got = back[b, :, cols(c)]
        return jnp.dot(share[b, 0], got, preferred_element_type=jnp.float32) + jnp.dot(
            share[b, 1], got, preferred_element_type=jnp.float32
        )

    def sum_copy(b, way, c):
        return remote(
            sums.at[b, :, cols(c)],
            came.at[way, b, :, cols(c)],
            sum_send.at[b, c],
            sum_recv.at[way, b, c],
            toward(way),
        )

    cut = 256

    def answers(b, c):
        for d in range(1, g.peers):
            ans_copy(b, d, c).start()
        ans_own_copy(b, c).start()

    def expert(b, reply=True):
        for c in range(parts):
            own_copy(b, c).wait()
            for d in range(1, g.peers):
                row_copy(b, d, c).wait_recv()

        def inner(n, carry):
            at = pl.ds(pl.multiple_of(n * cut, cut), cut)
            x = out[b]
            gate = jnp.dot(x, v_gate[:, at], preferred_element_type=jnp.float32)
            upper = jnp.dot(x, v_up[:, at], preferred_element_type=jnp.float32)
            hidden[:, at] = (gate * jax.nn.sigmoid(gate) * upper).astype(jnp.bfloat16)
            return carry

        lax.fori_loop(0, v_gate.shape[1] // cut, inner, 0)
        for c in range(parts):
            answer = jnp.dot(hidden[...], v_down[:, cols(c)], preferred_element_type=jnp.float32)
            out[b, :, cols(c)] = answer.astype(jnp.bfloat16)
            if reply:
                answers(b, c)

    def reply_late(b):
        for c in range(parts):
            answers(b, c)

    def combine(way, b, c, relayed):
        total = partial(b, c)
        if relayed:
            sum_copy(b, way, c).wait_recv()
            total = total + came[way, b, :, cols(c)].astype(jnp.float32)
        sums[b, :, cols(c)] = total.astype(jnp.bfloat16)
        sum_copy(b, way, c).start()

    def arrive(b, c):
        if c == 0:
            table_copy(b, 0, False).wait_recv()
        block_copy(b, 0, c, False).wait_recv()
        place(b, c)
        if c == 0:
            weigh(b)

    def pass_on(b, way, c):
        if c == 0:
            table_copy(b, way, False).wait_recv()
            table_copy(b, way, False).start()
        block_copy(b, way, c, False).wait_recv()
        block_copy(b, way, c, False).start()
        place(b, c)
        if c == 0:
            weigh(b)

    def keep():
        for c in range(parts):
            h2[:, cols(c)] = residual_scale * first[:, cols(c)].astype(jnp.float32) + partial(plane, c)

    for way in range(2):

        @pl.when(has_way(way))
        def _():
            table_copy(plane, way, True).start()
            for c in range(parts):
                block_copy(plane, way, c, True).start()

    for c in range(parts):
        place(plane, c)
    weigh(plane)

    @pl.when(at_end)
    def _():
        low = plane == 0

        def other(s):
            return jnp.where(low, s, last - s)

        def send_back(s, c):
            for way in range(2):
                pl.when(low if way == 0 else jnp.logical_not(low))(lambda: combine(way, other(s), c, False))

        for c in range(parts):
            arrive(other(1), c)
        for load in loads:
            load.wait()
        expert(plane, False)
        for s in range(2, g.planes + 1):
            early = min(s - 1, 2) if s < g.planes else parts
            for c in range(early):
                if s < g.planes:
                    arrive(other(s), c)
            expert(other(s - 1))
            if s == g.planes:
                reply_late(plane)
            for c in range(early, parts):
                arrive(other(s), c)
                if s == 2:
                    send_back(s - 1, c - early)
            for c in range(parts - early if s == 2 else 0, parts):
                send_back(s - 1, c)
        keep()

    @pl.when(jnp.logical_not(at_end))
    def _():
        low = plane == 1
        far = jnp.where(low, last, 0)
        close = jnp.where(low, 2, 1)
        end = jnp.where(low, 0, last)

        def pass_far(c):
            for way in range(2):
                pl.when(low if way == 1 else jnp.logical_not(low))(lambda: pass_on(far, way, c))

        def sums_for(b, up, c):
            for way in range(2):
                pl.when(up if way == 0 else jnp.logical_not(up))(lambda: combine(way, b, c, True))

        for c in range(parts):
            pass_on(plane - 1, 0, c)
            pass_on(plane + 1, 1, c)
        for load in loads:
            load.wait()
        expert(plane, False)
        pass_far(0)
        expert(close)
        pass_far(1)
        pass_far(2)
        expert(end, False)
        pass_far(3)
        expert(far)
        reply_late(end)
        reply_late(plane)
        for c in range(parts):
            sums_for(close, low, c)
        for c in range(parts + 1):
            if c < parts:
                sums_for(far, low, c)
            if c == parts - 1:
                keep()
            if c > 0:
                sums_for(end, jnp.logical_not(low), c - 1)

    for c in range(parts):
        for way in range(2):

            @pl.when(plane > 0 if way == 0 else plane < last)
            def _():
                sum_copy(plane, way, c).wait_recv()
                h2[:, cols(c)] += came[way, plane, :, cols(c)].astype(jnp.float32)

    final[...] = token_norm(h2[...], gain[...]).astype(jnp.bfloat16)
    for c in range(parts):
        for b in range(g.planes):
            pl.when(plane != b)(lambda: sum_copy(b, 0, c).wait_send())
        for b in range(g.planes):
            for d in range(1, g.peers):
                ans_copy(b, d, c).wait_send()
                row_copy(b, d, c).wait_send()
        for s in range(1, g.planes):
            for way, b, valid in near(s):
                pl.when(valid & has_way(way))(lambda: block_copy(b, way, c, False).wait_send())
        for way in range(2):
            pl.when(has_way(way))(lambda: block_copy(plane, way, c, True).wait_send())
    for s in range(1, g.planes):
        for way, b, valid in near(s):
            pl.when(valid & has_way(way))(lambda: table_copy(b, way, False).wait_send())
    for way in range(2):
        pl.when(has_way(way))(lambda: table_copy(plane, way, True).wait_send())


def experts(g, cap, first, table, gain, w_gate, w_up, w_down):
    rows, width = first.shape
    hidden = w_gate.shape[2]
    slots = g.peers * cap
    parts = 4
    dma = pltpu.SemaphoreType.DMA
    f32, bf16 = jnp.float32, jnp.bfloat16
    blocks, pairs = dma((g.planes, parts)), dma((g.planes, g.peers, parts))
    any_place = pl.BlockSpec(memory_space=pl.ANY)
    return pl.pallas_call(
        functools.partial(experts_kernel, g, cap, parts),
        name="experts",
        out_shape=jax.ShapeDtypeStruct((rows, width), bf16),
        in_specs=[VMEM] * 3 + [any_place] * 3,
        out_specs=VMEM,
        scratch_shapes=[
            pltpu.VMEM((width, hidden), bf16),
            pltpu.VMEM((width, hidden), bf16),
            pltpu.VMEM((hidden, width), bf16),
            pltpu.VMEM((slots, hidden), bf16),
            pltpu.VMEM((g.planes, slots, width), bf16),
            pltpu.VMEM((g.planes,) + table.shape, f32),
            pltpu.VMEM((g.planes, rows, width), bf16),
            pltpu.VMEM((g.planes, slots, width), bf16),
            pltpu.VMEM((g.planes, slots, width), bf16),
            pltpu.VMEM((g.planes, rows, width), bf16),
            pltpu.VMEM((2, g.planes, rows, width), bf16),
            pltpu.VMEM((rows, width), f32),
            pltpu.VMEM((g.planes, 2, rows, slots), bf16),
            dma((2, g.planes, parts)),
            blocks,
            dma((2, g.planes)),
            dma((g.planes,)),
            pairs,
            pairs,
            blocks,
            pairs,
            pairs,
            blocks,
            blocks,
            dma((2, g.planes, parts)),
            dma((3,)),
        ],
        compiler_params=pltpu.CompilerParams(collective_id=0, has_side_effects=True),
    )(first, table, gain, w_gate, w_up, w_down)


def front_kernel(
    sp, tp, value, gate, taps, gain, out, rim_v, rim_g, glu, conv, part1, part2, stat, stats, cols, stage,
    rim_send, rim_recv, stat_send, stat_recv, act_send, act_recv, own_sem,
):
    s, t = lax.axis_index("sp"), lax.axis_index("tp")
    tokens, width = value.shape
    kw = taps.shape[0]
    pad = rim_v.shape[0]
    rows = tokens // tp
    lead = pad - (kw - 1)
    tile = 64
    lane = 128

    barrier = pltpu.get_barrier_semaphore()
    for other in ((s + 1) % sp, (s + sp - 1) % sp):
        pl.semaphore_signal(barrier, inc=1, device_id=(other, t), device_id_type=MESH)
    for d in range(1, tp):
        pl.semaphore_signal(barrier, inc=1, device_id=(s, (t + d) % tp), device_id_type=MESH)
    pl.semaphore_wait(barrier, 2 + tp - 1)

    def rims():
        to = ((s + 1) % sp, t)
        tail = pl.ds(tokens - pad, pad)
        return (
            remote(value.at[tail], rim_v, rim_send.at[0], rim_recv.at[0], to),
            remote(gate.at[tail], rim_g, rim_send.at[1], rim_recv.at[1], to),
        )

    @pl.when(s < sp - 1)
    def _():
        for copy in rims():
            copy.start()

    def gated(v, g):
        return v.astype(jnp.float32) * jax.nn.sigmoid(g.astype(jnp.float32))

    def glu_tile(i, carry):
        at = pl.multiple_of(i * tile, tile)
        glu[pl.ds(pad + at, tile)] = gated(value[pl.ds(at, tile)], gate[pl.ds(at, tile)])
        return carry

    lax.fori_loop(0, tokens // tile, glu_tile, 0)

    def conv_tile(i, carry):
        at = pl.multiple_of(i * tile, tile)
        one = two = None
        for c in range(width // lane):
            lanes = pl.ds(c * lane, lane)
            total = None
            for r in range(8):
                piece = None
                extra = 8 if r else 0
                for m in range(pad // 8 + 1):
                    j = 8 * m + r - lead
                    if 0 <= j < kw:
                        term = taps[j : j + 1, lanes] * glu[pl.ds(at + 8 * m, tile + extra), lanes]
                        piece = term if piece is None else piece + term
                if piece is not None:
                    piece = piece[r : r + tile]
                    total = piece if total is None else total + piece
            conv[pl.ds(at, tile), lanes] = total
            one = total if one is None else one + total
            two = total * total if two is None else two + total * total
        part1[pl.ds(at, tile)] = one
        part2[pl.ds(at, tile)] = two
        return carry

    lax.fori_loop(1, tokens // tile, conv_tile, 0)

    @pl.when(s > 0)
    def _():
        for copy in rims():
            copy.wait_recv()
        glu[pl.ds(0, pad)] = gated(rim_v[...], rim_g[...])

    @pl.when(s == 0)
    def _():
        glu[pl.ds(0, pad)] = jnp.zeros((pad, width), jnp.float32)

    conv_tile(0, 0)

    ones = jnp.ones((8, lane), jnp.float32)

    def row_sums(part):
        return lax.dot_general(
            ones,
            part[...],
            (((1,), (1,)), ((), ())),
            precision=lax.Precision.HIGHEST,
            preferred_element_type=jnp.float32,
        )

    first_row = lax.broadcasted_iota(jnp.int32, (8, tokens), 0) == 0
    mine = jnp.where(first_row, row_sums(part1), row_sums(part2))
    stat[...] = mine

    def stat_copy(d):
        return remote(stat, stats.at[d], stat_send.at[d], stat_recv.at[d], (s, (t + d) % tp))

    for d in range(1, tp):
        stat_copy(d).start()
    for d in range(1, tp):
        stat_copy(d).wait_recv()
        mine = mine + stats[d]
    scaled = mine / (width * tp)
    middle = scaled[0:1]
    factor = lax.rsqrt(scaled[1:2] - middle * middle + 1e-05)
    cols[...] = jnp.where(first_row, middle, factor).T

    def act_copy(d):
        to = (t + d) % tp
        return remote(
            stage.at[d],
            out.at[:, pl.ds(pl.multiple_of(t * width, width), width)],
            act_send.at[d],
            act_recv.at[d],
            (s, to),
        )

    own = pltpu.make_async_copy(stage.at[0], out.at[:, pl.ds(pl.multiple_of(t * width, width), width)], own_sem)
    for d in list(range(1, tp)) + [0]:
        at = pl.multiple_of((t + d) % tp * rows, rows)
        side = cols[pl.ds(at, rows)]
        normed = (conv[pl.ds(at, rows)] - side[:, 0:1]) * side[:, 1:2] * gain[...]
        stage[d] = (normed * jax.nn.sigmoid(normed)).astype(jnp.bfloat16)
        if d:
            act_copy(d).start()
        else:
            own.start()
    own.wait()
    for d in range(1, tp):
        act_copy(d).wait()
        stat_copy(d).wait_send()

    @pl.when(s < sp - 1)
    def _():
        for copy in rims():
            copy.wait_send()


def front(sp, tp, value, gate, taps, gain):
    tokens, width = value.shape
    pad = -(-(taps.shape[0] - 1) // 16) * 16
    rows = tokens // tp
    dma = pltpu.SemaphoreType.DMA
    f32, bf16 = jnp.float32, jnp.bfloat16
    return pl.pallas_call(
        functools.partial(front_kernel, sp, tp),
        name="front",
        out_shape=jax.ShapeDtypeStruct((rows, width * tp), bf16),
        in_specs=[VMEM] * 4,
        out_specs=VMEM,
        scratch_shapes=[
            pltpu.VMEM((pad, width), bf16),
            pltpu.VMEM((pad, width), bf16),
            pltpu.VMEM((pad + tokens, width), f32),
            pltpu.VMEM((tokens, width), f32),
            pltpu.VMEM((tokens, 128), f32),
            pltpu.VMEM((tokens, 128), f32),
            pltpu.VMEM((8, tokens), f32),
            pltpu.VMEM((tp, 8, tokens), f32),
            pltpu.VMEM((tokens, 8), f32),
            pltpu.VMEM((tp, rows, width), bf16),
            dma((2,)),
            dma((2,)),
            dma((tp,)),
            dma((tp,)),
            dma((tp,)),
            dma((tp,)),
            dma,
        ],
        compiler_params=pltpu.CompilerParams(collective_id=2, has_side_effects=True),
    )(value, gate, taps, gain)


def token_norm(values, gain):
    middle = jnp.mean(values, axis=-1, keepdims=True)
    centred = values - middle
    spread = jnp.mean(centred * centred, axis=-1, keepdims=True)
    return centred * lax.rsqrt(spread + 1e-05) * gain


def per_device(
    conv_value,
    conv_gate,
    conv_taps,
    channel_gain,
    point_weight,
    residual_in,
    first_gain,
    second_gain,
    routes,
    route_score,
    expert_gate,
    expert_up,
    expert_down,
):
    owned = front(
        lax.axis_size("sp"), lax.axis_size("tp"), conv_value, conv_gate, conv_taps, channel_gain[None]
    )
    rows = owned.shape[0]
    mix = jnp.dot(owned, point_weight, preferred_element_type=jnp.float32)
    first = token_norm(residual_scale * residual_in.astype(jnp.float32) + mix, first_gain).astype(
        jnp.bfloat16
    )
    top = routes.shape[1]
    g = Grid(lax.axis_size("sp"), lax.axis_size("tp"))
    count = g.planes * g.peers
    most = max(2, 2 * rows * top // count)
    cap = -(-most // 16) * 16
    flat_e = routes.reshape(-1)
    onehot = (flat_e[:, None] == jnp.arange(count, dtype=jnp.int32)[None, :]).astype(jnp.int32)
    before = jnp.sum((jnp.cumsum(onehot, axis=0) - onehot) * onehot, axis=1)
    slot = (flat_e * cap + before).reshape(rows, top).astype(jnp.float32)
    share = route_score / jnp.sum(route_score, axis=1, keepdims=True)
    table = jnp.concatenate([slot, share, jnp.zeros((rows, 4), jnp.float32)], axis=1).T
    return experts(g, cap, first, table, second_gain[None], expert_gate, expert_up, expert_down)


def solution(mesh):
    in_specs = (
        P("sp", "tp"),
        P("sp", "tp"),
        P(None, "tp"),
        P("tp"),
        P(),
        P(("sp", "tp"), None),
        P(),
        P(),
        P(("sp", "tp"), None),
        P(("sp", "tp"), None),
        P(("sp", "tp"), None, None),
        P(("sp", "tp"), None, None),
        P(("sp", "tp"), None, None),
    )
    out_specs = P(("sp", "tp"), None)
    return jax.shard_map(
        per_device, mesh=mesh, in_specs=in_specs, out_specs=out_specs, check_vma=False
    )
```
